32 devices in a mesh: ra: 8 (over z, y), cb: 4 (over x, core).
Axes of the slice: x: 2, y: 2, z: 4, core: 2. Of those that a mesh axis runs over, the one named last changes fastest.
Arguments:
- tokens: bfloat16 [4, 128, 4096], P(None, None, 'ra'), may hold values from -64 to 64
- norm_gain: float32 [2, 4096], P(None, 'ra'), may hold values from 0.1 to 1.9
- gate_weight: bfloat16 [2, 4096, 11264], P(None, 'ra', 'cb'), may hold values from -0.09375 to 0.09375
- up_weight: bfloat16 [2, 4096, 11264], P(None, 'ra', 'cb'), may hold values from -0.09375 to 0.09375
- gate_taps: float32 [2, 3, 11264], P(None, None, 'cb'), may hold values from -3 to 3
- up_taps: float32 [2, 3, 11264], P(None, None, 'cb'), may hold values from -3 to 3
- gate_bias: float32 [2, 11264], P(None, 'cb'), may hold values from -3 to 3
- up_bias: float32 [2, 11264], P(None, 'cb'), may hold values from -3 to 3
- down_weight: bfloat16 [2, 11264, 4096], P(None, 'cb', 'ra'), may hold values from -0.0546875 to 0.0546875
Outputs:
- mixed: bfloat16 [4, 128, 4096], P(None, None, 'ra')
The draws below stay inside these ranges and needn't reach their ends.
All inputs are finite; a program needn't handle non-finite values.
Results may differ from the reference program's by a relative error of at most 0.03.
Values may be sent and summed in bfloat16 or wider, within the bound.
A program may use at most 64 MiB of HBM per device.

```python
import jax
import jax.numpy as jnp
from jax import lax

D = 4096
FF = 11264
KERNEL = 3
LAYERS = 2
SEQS = 4
LEN = 128


def draw_tokens(key, part):
    key_base, key_scale, key_rows, key_common = jax.random.split(key, 4)
    width = D // 32
    noise = jnp.clip(jax.random.normal(key_base, (SEQS, LEN, D), jnp.float32), -6.0, 6.0)
    row_scale = jnp.exp(jax.random.uniform(key_rows, (SEQS, LEN, 1), jnp.float32, -0.5, 0.5))
    scales = jnp.exp(jax.random.uniform(key_scale, (32,), jnp.float32, -1.4, 1.4))
    columns = jnp.repeat(scales, width)
    return jnp.clip(noise * columns * row_scale, -64.0, 64.0).astype(jnp.bfloat16)


def block_scale(rng, shape, cuts, least, largest):
    loudness = 1.0
    for position, parts in cuts:
        heights = jax.random.uniform(jax.random.fold_in(jax.random.fold_in(rng, 6), position), (parts,), jnp.float32, least / len(cuts), largest / len(cuts))
        loudness = loudness * jnp.repeat(jnp.exp(heights), shape[position] // parts).reshape((-1,) + (1,) * (len(shape) - 1 - position))
    return loudness


def centred(stream_key, shape, deviation, most, shards=(), dtype=jnp.bfloat16):
    gain = block_scale(stream_key, shape, shards, -0.22, 0.18) if shards else 1.0
    values = jax.random.normal(stream_key, shape, jnp.float32) * deviation * gain
    return jnp.minimum(jnp.maximum(values, -most), most).astype(dtype)


def setup_inputs(seed: int = 0) -> dict:
    arg_keys = jax.random.split(jax.random.key(seed), 10)
    tokens = draw_tokens(jax.random.fold_in(arg_keys[9], 71), 0)
    norm_gain = jnp.clip(1.0 + 0.18 * jax.random.normal(arg_keys[1], (LAYERS, D), jnp.float32), 0.1, 1.9)
    gate_weight = centred(arg_keys[2], (LAYERS, D, FF), D ** -0.5, 0.09375, ((1, 8), (2, 4)))
    up_weight = centred(arg_keys[3], (LAYERS, D, FF), D ** -0.5, 0.09375, ((1, 8), (2, 4)))
    gate_taps = centred(arg_keys[4], (LAYERS, KERNEL, FF), 0.6, 3.0, ((2, 4),), jnp.float32)
    up_taps = centred(arg_keys[5], (LAYERS, KERNEL, FF), 0.6, 3.0, ((2, 4),), jnp.float32)
    gate_bias = centred(arg_keys[6], (LAYERS, FF), 0.5, 3.0, ((1, 4),), jnp.float32)
    up_bias = centred(arg_keys[7], (LAYERS, FF), 0.5, 3.0, ((1, 4),), jnp.float32)
    down_weight = centred(arg_keys[8], (LAYERS, FF, D), FF ** -0.5, 0.0546875, ((1, 4), (2, 8)))
    return {"tokens": tokens, "norm_gain": norm_gain, "gate_weight": gate_weight, "up_weight": up_weight, "gate_taps": gate_taps, "up_taps": up_taps, "gate_bias": gate_bias, "up_bias": up_bias, "down_weight": down_weight}


eps = 1e-06
resid_scale = 0.5

def causal_conv(projected, kernel, offsets):
    values = projected.astype(jnp.float32).reshape(SEQS, LEN, FF)
    padded = jnp.pad(values, ((0, 0), (KERNEL - 1, 0), (0, 0)))
    result = offsets
    for tap_idx in range(KERNEL):
        result = result + kernel[tap_idx] * padded[:, tap_idx:tap_idx + LEN]
    return result.reshape(SEQS * LEN, FF)

def reference(tokens, norm_gain, gate_weight, up_weight, gate_taps, up_taps, gate_bias, up_bias, down_weight):
    carried = tokens.reshape(SEQS * LEN, D).astype(jnp.float32)
    for layer_idx in range(LAYERS):
        row_squares = lax.optimization_barrier(jnp.sum(carried * carried, axis=1))
        scaled = (carried * norm_gain[layer_idx]).astype(jnp.bfloat16)
        inverse = lax.rsqrt(row_squares / D + eps)
        gate_pre = (jnp.dot(scaled, gate_weight[layer_idx], preferred_element_type=jnp.float32) * inverse[:, None]).astype(jnp.bfloat16)
        up_pre = (jnp.dot(scaled, up_weight[layer_idx], preferred_element_type=jnp.float32) * inverse[:, None]).astype(jnp.bfloat16)
        gate_conv = causal_conv(gate_pre, gate_taps[layer_idx], gate_bias[layer_idx])
        up_conv = causal_conv(up_pre, up_taps[layer_idx], up_bias[layer_idx])
        hidden = (jax.nn.silu(gate_conv) * up_conv).astype(jnp.bfloat16)
        branch = jnp.dot(hidden, down_weight[layer_idx], preferred_element_type=jnp.float32)
        carried = resid_scale * carried + branch
    return carried.astype(jnp.bfloat16).reshape(SEQS, LEN, D)
```

```python
import functools

import jax
import jax.numpy as jnp
from jax import lax
from jax.experimental import pallas as pl
from jax.experimental.pallas import tpu as pltpu
from jax.sharding import PartitionSpec as P

EPS = 1e-06
RESID = 0.5
LAG_B, LAG_C, LAG_D, LAG_E = 1, 3, 5, 6

MESH = pl.DeviceIdType.MESH
F32, BF16 = jnp.float32, jnp.bfloat16


def kernel(
    dims,
    tok_ref, gain_ref, gw_hbm, uw_hbm, gt_ref, ut_ref, gb_ref, ub_ref, dw_hbm,
    out_ref,
    gw_ref, uw_ref, dw_ref, carried, scaled, inv, tmp, acc,
    sq_own, sq_in, part, y_in, zpart, z_in, hid, c_out, c_in, c_all,
    w_sem, sq_s, sq_r, y_s, y_r, z_s, z_r, hz_s, hz_r, hy_s, hy_r, c_s, c_r, ca_s, ca_r,
):
    n_ra, n_cb, nz, seqs, length, layers, width, chunks = dims
    ny = n_ra // nz
    rows = seqs * length
    part_rows = length // ny
    cb_rows = rows // n_cb
    me_ra = lax.axis_index("ra")
    me_cb = lax.axis_index("cb")
    me_z, me_y = me_ra // ny, me_ra % ny

    def weight_copies(layer):
        return [
            pltpu.make_async_copy(src.at[layer], dst.at[layer], w_sem.at[layer, k])
            for k, (src, dst) in enumerate(
                [(gw_hbm, gw_ref), (uw_hbm, uw_ref), (dw_hbm, dw_ref)]
            )
        ]

    for layer in range(layers):
        for copy in weight_copies(layer):
            copy.start()

    barrier = pltpu.get_barrier_semaphore()
    for step in range(1, n_ra):
        pl.semaphore_signal(
            barrier, inc=1, device_id={"ra": lax.rem(me_ra + step, n_ra)}, device_id_type=MESH
        )
    for step in range(1, n_cb):
        pl.semaphore_signal(
            barrier, inc=1, device_id={"cb": lax.rem(me_cb + step, n_cb)}, device_id_type=MESH
        )
    pl.semaphore_wait(barrier, n_ra + n_cb - 2)

    def remote(src, dst, send, recv, **where):
        return pltpu.make_async_remote_copy(
            src_ref=src, dst_ref=dst, send_sem=send, recv_sem=recv,
            device_id=where, device_id_type=MESH,
        )

    def square_copy(step):
        return remote(
            sq_own, sq_in.at[step - 1], sq_s.at[step - 1], sq_r.at[step - 1],
            ra=lax.rem(me_ra + step, n_ra),
        )

    def y_copy(i, step):
        to = lax.rem(me_y + step, ny)
        return remote(
            part.at[i, to], y_in.at[i, step - 1], y_s.at[i, step - 1], y_r.at[i, step - 1],
            ra=me_z * ny + to,
        )

    def z_copy(i, step):
        to = lax.rem(me_z + step, nz)
        return remote(
            zpart.at[i, to], z_in.at[i, step - 1], z_s.at[i, step - 1], z_r.at[i, step - 1],
            ra=to * ny + me_y,
        )

    def hz_copy(i, step, z):
        to = lax.rem(me_z + step, nz)
        block = hid.at[i, me_y, z]
        return remote(
            block, block, hz_s.at[i, step - 1], hz_r.at[i, step - 1], ra=to * ny + me_y
        )

    def hy_copy(i, step, y):
        to = lax.rem(me_y + step, ny)
        block = hid.at[i, y]
        return remote(
            block, block, hy_s.at[i, step - 1], hy_r.at[i, step - 1], ra=me_z * ny + to
        )

    def c_copy(step):
        to = lax.rem(me_cb + step, n_cb)
        return remote(c_out.at[to], c_in.at[step - 1], c_s.at[step - 1], c_r.at[step - 1], cb=to)

    def ca_copy(step, block):
        to = lax.rem(me_cb + step, n_cb)
        return remote(
            c_all.at[block], c_all.at[block], ca_s.at[step - 1], ca_r.at[step - 1], cb=to
        )

    carried[...] = tok_ref[...].astype(F32)
    row_in_seq = lax.broadcasted_iota(jnp.int32, (length, width), 0)

    def one_layer(layer, _):
        values = carried[...]
        squares = jnp.sum(values * values, axis=1, keepdims=True)
        sq_own[...] = jnp.transpose(jnp.broadcast_to(squares, (rows, 128)))[:8]
        for step in range(1, n_ra):
            square_copy(step).start()
        scaled[...] = (values * gain_ref[layer]).astype(BF16)
        acc[...] = jnp.zeros_like(acc)
        for copy in weight_copies(layer):
            copy.wait()
        total = sq_own[...]
        for step in range(1, n_ra):
            square_copy(step).wait()
            total = total + sq_in[step - 1]
        total = jnp.transpose(jnp.concatenate([total] * 16, axis=0))
        inv[...] = lax.rsqrt(total / (n_ra * gain_ref.shape[2]) + EPS)

        def project(i):
            cols = pl.ds(pl.multiple_of(i * width, width), width)
            for half, (w_ref, taps) in enumerate([(gw_ref, gt_ref), (uw_ref, ut_ref)]):
                lanes = slice(half * width, (half + 1) * width)
                tmp[...] = jnp.dot(
                    scaled[...], w_ref[layer, :, cols], preferred_element_type=F32
                )
                tap = [taps[layer, pl.ds(k, 1), cols] for k in range(3)]
                for s in range(seqs):
                    span = slice(s * length, (s + 1) * length)
                    pre = tmp[span, :] * inv[span, :1]
                    last = jnp.where(row_in_seq >= 1, pltpu.roll(pre, 1, 0), 0.0)
                    older = jnp.where(row_in_seq >= 2, pltpu.roll(pre, 2, 0), 0.0)
                    conv = (tap[0] * older + tap[1] * last + tap[2] * pre).astype(BF16)
                    for y in range(ny):
                        part[i, y, s, :, lanes] = conv[y * part_rows : (y + 1) * part_rows]
            for step in range(1, ny):
                y_copy(i, step).start()

        def add_y(i):
            for step in range(1, ny):
                y_copy(i, step).wait_recv()
            for s in range(seqs):
                value = part[i, me_y, s].astype(F32)
                for step in range(1, ny):
                    value = value + y_in[i, step - 1, s].astype(F32)
                zpart[i, s] = value.astype(BF16)
            for step in range(1, nz):
                z_copy(i, step).start()

        def activate(i):
            cols = pl.ds(pl.multiple_of(i * width, width), width)
            for step in range(1, nz):
                z_copy(i, step).wait_recv()
            value = zpart[i, me_z].astype(F32)
            for step in range(1, nz):
                value = value + z_in[i, step - 1].astype(F32)
            gate = value[:, :width] + gb_ref[layer, :, cols]
            up = value[:, width:] + ub_ref[layer, :, cols]
            hid[i, me_y, me_z] = (gate / (1.0 + jnp.exp(-gate)) * up).astype(BF16)
            for step in range(1, nz):
                hz_copy(i, step, me_z).start()

        def spread_y(i):
            for step in range(1, nz):
                hz_copy(i, step, lax.rem(me_z - step + nz, nz)).wait_recv()
            for step in range(1, ny):
                hy_copy(i, step, me_y).start()

        def down(i):
            depth = pl.ds(pl.multiple_of(i * width, width), width)
            for step in range(1, ny):
                hy_copy(i, step, lax.rem(me_y - step + ny, ny)).wait_recv()
            acc[...] += jnp.dot(
                hid[i].reshape(rows, width), dw_ref[layer, depth, :], preferred_element_type=F32
            )

        def body(t, _):
            for lag, stage in [
                (0, project), (LAG_B, add_y), (LAG_C, activate), (LAG_D, spread_y), (LAG_E, down)
            ]:
                i = t - lag

                @pl.when((i >= 0) & (i < chunks))
                def _():
                    stage(i)

            return 0

        lax.fori_loop(0, chunks + LAG_E, body, 0)

        c_out[...] = acc[...].astype(BF16).reshape(c_out.shape)
        for step in range(1, n_cb):
            c_copy(step).start()

        def settle(i, _):
            for step in range(1, ny):
                y_copy(i, step).wait_send()
                hy_copy(i, step, me_y).wait_send()
            for step in range(1, nz):
                z_copy(i, step).wait_send()
                hz_copy(i, step, me_z).wait_send()
            return 0

        lax.fori_loop(0, chunks, settle, 0)

        value = acc[pl.ds(pl.multiple_of(me_cb * cb_rows, cb_rows), cb_rows), :]
        for step in range(1, n_cb):
            c_copy(step).wait()
            value = value + c_in[step - 1].astype(F32)
        c_all[me_cb] = value.astype(BF16)
        for step in range(1, n_cb):
            ca_copy(step, me_cb).start()
        for step in range(1, n_cb):
            ca_copy(step, lax.rem(me_cb - step + n_cb, n_cb)).wait_recv()
            ca_copy(step, me_cb).wait_send()
        branch = c_all[...].reshape(rows, c_all.shape[2]).astype(F32)
        for y in range(ny):
            for s in range(seqs):
                to = slice(s * length + y * part_rows, s * length + (y + 1) * part_rows)
                at = (y * seqs + s) * part_rows
                carried[to, :] = RESID * carried[to, :] + branch[at : at + part_rows]
        return 0

    lax.fori_loop(0, layers, one_layer, 0)
    out_ref[...] = carried[...].astype(out_ref.dtype)


def per_device(n_ra, n_cb, tokens, gain, gw, uw, gt, ut, gb, ub, dw):
    seqs, length, d = tokens.shape
    layers, _, ff = gw.shape
    rows = seqs * length
    nz = seqs
    ny = n_ra // nz
    pr = length // ny
    width = 256 if ff % 256 == 0 and ff // 256 >= 8 else 128
    chunks = ff // width
    dims = (n_ra, n_cb, nz, seqs, length, layers, width, chunks)
    vmem = pl.BlockSpec(memory_space=pltpu.VMEM)
    hbm = pl.BlockSpec(memory_space=pl.ANY)
    dma = pltpu.SemaphoreType.DMA
    ys, zs = max(ny - 1, 1), nz - 1
    scratch = [
        pltpu.VMEM((layers, d, ff), BF16),
        pltpu.VMEM((layers, d, ff), BF16),
        pltpu.VMEM((layers, ff, d), BF16),
        pltpu.VMEM((rows, d), F32),
        pltpu.VMEM((rows, d), BF16),
        pltpu.VMEM((rows, 128), F32),
        pltpu.VMEM((rows, width), F32),
        pltpu.VMEM((rows, d), F32),
        pltpu.VMEM((8, rows), F32),
        pltpu.VMEM((n_ra - 1, 8, rows), F32),
        pltpu.VMEM((chunks, ny, seqs, pr, 2 * width), BF16),
        pltpu.VMEM((chunks, ys, seqs, pr, 2 * width), BF16),
        pltpu.VMEM((chunks, seqs, pr, 2 * width), BF16),
        pltpu.VMEM((chunks, zs, pr, 2 * width), BF16),
        pltpu.VMEM((chunks, ny, seqs, pr, width), BF16),
        pltpu.VMEM((n_cb, rows // n_cb, d), BF16),
        pltpu.VMEM((n_cb - 1, rows // n_cb, d), BF16),
        pltpu.VMEM((n_cb, rows // n_cb, d), BF16),
        dma((layers, 3)),
        dma((n_ra - 1,)), dma((n_ra - 1,)),
        dma((chunks, ys)), dma((chunks, ys)),
        dma((chunks, zs)), dma((chunks, zs)),
        dma((chunks, zs)), dma((chunks, zs)),
        dma((chunks, ys)), dma((chunks, ys)),
        dma((n_cb - 1,)), dma((n_cb - 1,)),
        dma((n_cb - 1,)), dma((n_cb - 1,)),
    ]
    out = pl.pallas_call(
        functools.partial(kernel, dims),
        out_shape=jax.ShapeDtypeStruct((rows, d), tokens.dtype),
        in_specs=[vmem, vmem, hbm, hbm, vmem, vmem, vmem, vmem, hbm],
        out_specs=vmem,
        scratch_shapes=scratch,
        compiler_params=pltpu.CompilerParams(
            collective_id=0, has_side_effects=True, vmem_limit_bytes=60 * 1024 * 1024
        ),
        name="blocks",
    )(
        tokens.reshape(rows, d), gain[:, None, :], gw, uw, gt, ut,
        gb[:, None, :], ub[:, None, :], dw,
    )
    return out.reshape(tokens.shape)


def solution(mesh):
    in_specs = (
        P(None, None, "ra"),
        P(None, "ra"),
        P(None, "ra", "cb"),
        P(None, "ra", "cb"),
        P(None, None, "cb"),
        P(None, None, "cb"),
        P(None, "cb"),
        P(None, "cb"),
        P(None, "cb", "ra"),
    )
    return jax.shard_map(
        functools.partial(per_device, mesh.shape["ra"], mesh.shape["cb"]),
        mesh=mesh, in_specs=in_specs, out_specs=P(None, None, "ra"), check_vma=False,
    )
```

```python
import functools

import jax
import jax.numpy as jnp
from jax import lax
from jax.experimental import pallas as pl
from jax.experimental.pallas import tpu as pltpu
from jax.sharding import PartitionSpec as P

EPS = 1e-06
RESID = 0.5
GROUPS = 2
STAGES = (("project", 0), ("add_y", 1), ("activate", 3), ("spread_y", 4), ("down", 6))
STAGES = tuple((lag, stage) for stage, lag in STAGES)
TAILS = ((0, "reduce_start"), (1, "reduce_end"), (2, "finish"), (3, "settle"))

MESH = pl.DeviceIdType.MESH
F32, BF16 = jnp.float32, jnp.bfloat16


def kernel(
    dims,
    tok_ref, gain_ref, gw_hbm, uw_hbm, gt_ref, ut_ref, gb_ref, ub_ref, dw_hbm,
    out_ref,
    gw_ref, uw_ref, dw_ref, carried, scaled, inv, tmp, acc,
    sq_own, sq_in, part, y_in, zpart, z_in, hid, c_out, c_in, c_all,
    w_sem, sq_s, sq_r, y_s, y_r, z_s, z_r, hz_s, hz_r, hy_s, hy_r, c_s, c_r, ca_s, ca_r,
):
    n_ra, n_cb, nz, groups, rows, length, layers, width, chunks = dims
    ny = n_ra // nz
    total_chunks = layers * groups * chunks
    cb_rows = rows // n_cb
    me_ra = lax.axis_index("ra")
    me_cb = lax.axis_index("cb")
    me_z, me_y = me_ra // ny, me_ra % ny

    def weight_copies(layer):
        return [
            pltpu.make_async_copy(src.at[layer], dst.at[layer], w_sem.at[layer, k])
            for k, (src, dst) in enumerate(
                [(gw_hbm, gw_ref), (uw_hbm, uw_ref), (dw_hbm, dw_ref)]
            )
        ]

    for layer in range(layers):
        for copy in weight_copies(layer):
            copy.start()

    barrier = pltpu.get_barrier_semaphore()
    for step in range(1, n_ra):
        pl.semaphore_signal(
            barrier, inc=1, device_id={"ra": lax.rem(me_ra + step, n_ra)}, device_id_type=MESH
        )
    for step in range(1, n_cb):
        pl.semaphore_signal(
            barrier, inc=1, device_id={"cb": lax.rem(me_cb + step, n_cb)}, device_id_type=MESH
        )

    def remote(src, dst, send, recv, **where):
        return pltpu.make_async_remote_copy(
            src_ref=src, dst_ref=dst, send_sem=send, recv_sem=recv,
            device_id=where, device_id_type=MESH,
        )

    def square_copy(g, step):
        return remote(
            sq_own.at[g], sq_in.at[g, step - 1], sq_s.at[g, step - 1], sq_r.at[g, step - 1],
            ra=lax.rem(me_ra + step, n_ra),
        )

    def y_copy(g, i, step):
        to = lax.rem(me_y + step, ny)
        return remote(
            part.at[g, i, to], y_in.at[g, i, step - 1],
            y_s.at[g, i, step - 1], y_r.at[g, i, step - 1], ra=me_z * ny + to,
        )

    def z_copy(g, i, step):
        to = lax.rem(me_z + step, nz)
        return remote(
            zpart.at[g, i, to], z_in.at[g, i, step - 1],
            z_s.at[g, i, step - 1], z_r.at[g, i, step - 1], ra=to * ny + me_y,
        )

    def hz_copy(g, i, step, z):
        to = lax.rem(me_z + step, nz)
        block = hid.at[g, i, me_y, z]
        return remote(
            block, block, hz_s.at[g, i, step - 1], hz_r.at[g, i, step - 1], ra=to * ny + me_y
        )

    def hy_copy(g, i, step, y):
        to = lax.rem(me_y + step, ny)
        block = hid.at[g, i, y]
        return remote(
            block, block, hy_s.at[g, i, step - 1], hy_r.at[g, i, step - 1], ra=me_z * ny + to
        )

    def c_copy(g, step):
        to = lax.rem(me_cb + step, n_cb)
        return remote(
            c_out.at[g, to], c_in.at[g, step - 1], c_s.at[g, step - 1], c_r.at[g, step - 1], cb=to
        )

    def ca_copy(g, step, block):
        to = lax.rem(me_cb + step, n_cb)
        block = c_all.at[g, block]
        return remote(block, block, ca_s.at[g, step - 1], ca_r.at[g, step - 1], cb=to)

    row_in_seq = lax.broadcasted_iota(jnp.int32, (length, width), 0)

    def prepare(layer, g):
        values = carried[g]
        squares = jnp.sum(values * values, axis=1, keepdims=True)
        sq_own[g] = jnp.transpose(jnp.broadcast_to(squares, (rows, 128)))[:8]
        for step in range(1, n_ra):
            square_copy(g, step).start()
        scaled[g] = (values * gain_ref[layer]).astype(BF16)
        acc[g] = jnp.zeros(acc.shape[1:], F32)

    def scale(g):
        total = sq_own[g]
        for step in range(1, n_ra):
            square_copy(g, step).wait()
            total = total + sq_in[g, step - 1]
        total = jnp.transpose(jnp.concatenate([total] * 16, axis=0))
        inv[g] = lax.rsqrt(total / (n_ra * gain_ref.shape[2]) + EPS)

    def project(layer, g, i):
        cols = pl.ds(pl.multiple_of(i * width, width), width)
        for half, (w_ref, taps) in enumerate([(gw_ref, gt_ref), (uw_ref, ut_ref)]):
            lanes = slice(half * width, (half + 1) * width)
            tmp[...] = jnp.dot(scaled[g], w_ref[layer, :, cols], preferred_element_type=F32)
            tap = [taps[layer, pl.ds(k, 1), cols] for k in range(3)]
            for s in range(rows // length):
                span = slice(s * length, (s + 1) * length)
                pre = tmp[span, :] * inv[g, span, :1]
                last = jnp.where(row_in_seq >= 1, pltpu.roll(pre, 1, 0), 0.0)
                older = jnp.where(row_in_seq >= 2, pltpu.roll(pre, 2, 0), 0.0)
                tmp[span, :] = tap[0] * older + tap[1] * last + tap[2] * pre
            part[g, i, :, :, :, lanes] = tmp[...].astype(BF16).reshape(
                ny, nz, rows // n_ra, width
            )
        for step in range(1, ny):
            y_copy(g, i, step).start()

    def add_y(layer, g, i):
        for step in range(1, ny):
            y_copy(g, i, step).wait_recv()
        value = part[g, i, me_y].astype(F32)
        for step in range(1, ny):
            value = value + y_in[g, i, step - 1].astype(F32)
        zpart[g, i] = value.astype(BF16)
        for step in range(1, nz):
            z_copy(g, i, step).start()

    def activate(layer, g, i):
        cols = pl.ds(pl.multiple_of(i * width, width), width)
        for step in range(1, nz):
            z_copy(g, i, step).wait_recv()
        value = zpart[g, i, me_z].astype(F32)
        for step in range(1, nz):
            value = value + z_in[g, i, step - 1].astype(F32)
        gate = value[:, :width] + gb_ref[layer, :, cols]
        up = value[:, width:] + ub_ref[layer, :, cols]
        hid[g, i, me_y, me_z] = (gate / (1.0 + jnp.exp(-gate)) * up).astype(BF16)
        for step in range(1, nz):
            hz_copy(g, i, step, me_z).start()

    def spread_y(layer, g, i):
        for step in range(1, nz):
            hz_copy(g, i, step, lax.rem(me_z - step + nz, nz)).wait_recv()
        for step in range(1, ny):
            hy_copy(g, i, step, me_y).start()

    def down(layer, g, i):
        depth = pl.ds(pl.multiple_of(i * width, width), width)
        for step in range(1, ny):
            hy_copy(g, i, step, lax.rem(me_y - step + ny, ny)).wait_recv()
        acc[g] += jnp.dot(
            hid[g, i].reshape(rows, width), dw_ref[layer, depth, :], preferred_element_type=F32
        )

    def reduce_start(layer, g):
        c_out[g] = acc[g].astype(BF16).reshape(c_out.shape[1:])
        for step in range(1, n_cb):
            c_copy(g, step).start()

    def reduce_end(layer, g):
        value = acc[g, pl.ds(pl.multiple_of(me_cb * cb_rows, cb_rows), cb_rows), :]
        for step in range(1, n_cb):
            c_copy(g, step).wait()
            value = value + c_in[g, step - 1].astype(F32)
        c_all[g, me_cb] = value.astype(BF16)
        for step in range(1, n_cb):
            ca_copy(g, step, me_cb).start()

    def finish(layer, g):
        for step in range(1, n_cb):
            ca_copy(g, step, lax.rem(me_cb - step + n_cb, n_cb)).wait_recv()
            ca_copy(g, step, me_cb).wait_send()
        branch = c_all[g].reshape(rows, c_all.shape[3]).astype(F32)
        carried[g] = RESID * carried[g] + branch

        @pl.when(layer < layers - 1)
        def _():
            prepare(layer + 1, g)

    def settle(layer, g):
        def one(i, _):
            for step in range(1, ny):
                y_copy(g, i, step).wait_send()
                hy_copy(g, i, step, me_y).wait_send()
            for step in range(1, nz):
                z_copy(g, i, step).wait_send()
                hz_copy(g, i, step, me_z).wait_send()
            return 0

        lax.fori_loop(0, chunks, one, 0)

        @pl.when(layer < layers - 1)
        def _():
            scale(g)

    carried[...] = tok_ref[...].astype(F32)
    pl.semaphore_wait(barrier, n_ra + n_cb - 2)
    for g in range(groups):
        prepare(0, g)
    for layer in range(layers):
        for copy in weight_copies(layer):
            copy.wait()
    for g in range(groups):
        scale(g)

    def body(t, _):
        for lag, stage in STAGES:
            at = t - lag
            run = at // chunks

            @pl.when((at >= 0) & (at < total_chunks))
            def _():
                stage_of[stage](run // groups, run % groups, at % chunks)

        for lag, stage in TAILS:
            at = t - STAGES[-1][0] - lag
            run = at // chunks

            @pl.when((at >= 0) & (at < total_chunks) & (at % chunks == chunks - 1))
            def _():
                stage_of[stage](run // groups, run % groups)

        return 0

    stage_of = {
        "project": project, "add_y": add_y, "activate": activate, "spread_y": spread_y,
        "down": down, "reduce_start": reduce_start, "reduce_end": reduce_end,
        "finish": finish, "settle": settle,
    }
    lax.fori_loop(0, total_chunks + STAGES[-1][0] + TAILS[-1][0], body, 0)
    out_ref[...] = carried[...].astype(out_ref.dtype)


def per_device(n_ra, n_cb, tokens, gain, gw, uw, gt, ut, gb, ub, dw):
    seqs, length, d = tokens.shape
    layers, _, ff = gw.shape
    nz = seqs
    ny = n_ra // nz
    groups = GROUPS
    rows = seqs * length // groups
    pr = rows // n_ra
    width = 256 if ff % 256 == 0 and ff // 256 >= 8 else 128
    chunks = ff // width
    dims = (n_ra, n_cb, nz, groups, rows, length, layers, width, chunks)
    vmem = pl.BlockSpec(memory_space=pltpu.VMEM)
    hbm = pl.BlockSpec(memory_space=pl.ANY)
    dma = pltpu.SemaphoreType.DMA
    ys, zs = max(ny - 1, 1), nz - 1
    scratch = [
        pltpu.VMEM((layers, d, ff), BF16),
        pltpu.VMEM((layers, d, ff), BF16),
        pltpu.VMEM((layers, ff, d), BF16),
        pltpu.VMEM((groups, rows, d), F32),
        pltpu.VMEM((groups, rows, d), BF16),
        pltpu.VMEM((groups, rows, 128), F32),
        pltpu.VMEM((rows, width), F32),
        pltpu.VMEM((groups, rows, d), F32),
        pltpu.VMEM((groups, 8, rows), F32),
        pltpu.VMEM((groups, n_ra - 1, 8, rows), F32),
        pltpu.VMEM((groups, chunks, ny, nz, pr, 2 * width), BF16),
        pltpu.VMEM((groups, chunks, ys, nz, pr, 2 * width), BF16),
        pltpu.VMEM((groups, chunks, nz, pr, 2 * width), BF16),
        pltpu.VMEM((groups, chunks, zs, pr, 2 * width), BF16),
        pltpu.VMEM((groups, chunks, ny, nz, pr, width), BF16),
        pltpu.VMEM((groups, n_cb, rows // n_cb, d), BF16),
        pltpu.VMEM((groups, n_cb - 1, rows // n_cb, d), BF16),
        pltpu.VMEM((groups, n_cb, rows // n_cb, d), BF16),
        dma((layers, 3)),
        dma((groups, n_ra - 1)), dma((groups, n_ra - 1)),
        dma((groups, chunks, ys)), dma((groups, chunks, ys)),
        dma((groups, chunks, zs)), dma((groups, chunks, zs)),
        dma((groups, chunks, zs)), dma((groups, chunks, zs)),
        dma((groups, chunks, ys)), dma((groups, chunks, ys)),
        dma((groups, n_cb - 1)), dma((groups, n_cb - 1)),
        dma((groups, n_cb - 1)), dma((groups, n_cb - 1)),
    ]
    out = pl.pallas_call(
        functools.partial(kernel, dims),
        out_shape=jax.ShapeDtypeStruct((groups, rows, d), tokens.dtype),
        in_specs=[vmem, vmem, hbm, hbm, vmem, vmem, vmem, vmem, hbm],
        out_specs=vmem,
        scratch_shapes=scratch,
        compiler_params=pltpu.CompilerParams(
            collective_id=0, has_side_effects=True, vmem_limit_bytes=60 * 1024 * 1024
        ),
        name="blocks",
    )(
        tokens.reshape(groups, rows, d), gain[:, None, :], gw, uw, gt, ut,
        gb[:, None, :], ub[:, None, :], dw,
    )
    return out.reshape(tokens.shape)


def solution(mesh):
    in_specs = (
        P(None, None, "ra"),
        P(None, "ra"),
        P(None, "ra", "cb"),
        P(None, "ra", "cb"),
        P(None, None, "cb"),
        P(None, None, "cb"),
        P(None, "cb"),
        P(None, "cb"),
        P(None, "cb", "ra"),
    )
    return jax.shard_map(
        functools.partial(per_device, mesh.shape["ra"], mesh.shape["cb"]),
        mesh=mesh, in_specs=in_specs, out_specs=P(None, None, "ra"), check_vma=False,
    )
```

```python
import functools

import jax
import jax.numpy as jnp
from jax import lax
from jax.experimental import pallas as pl
from jax.experimental.pallas import tpu as pltpu
from jax.sharding import PartitionSpec as P

EPS = 1e-06
RESID = 0.5
GROUPS = 2
STAGES = (("project", 0), ("add_y", 2), ("fold", 3), ("activate", 4),
          ("spread_z", 5), ("spread_y", 6), ("down", 8))
STAGES = tuple((lag, stage) for stage, lag in STAGES)
TAILS = ((0, "reduce_start"), (1, "reduce_end"), (2, "finish"), (3, "settle"))

MESH = pl.DeviceIdType.MESH
F32, BF16 = jnp.float32, jnp.bfloat16


def kernel(
    dims,
    tok_ref, gain_ref, gw_hbm, uw_hbm, gt_ref, ut_ref, gb_ref, ub_ref, dw_hbm,
    out_ref,
    gw_ref, uw_ref, dw_ref, carried, scaled, inv, tmp, acc,
    sq_own, sq_in, part, y_in, zpart, z_in, zfold, zf_in, hid, c_out, c_in, c_all,
    w_sem, sq_s, sq_r, y_s, y_r, z_s, z_r, hz_s, hz_r, hy_s, hy_r, c_s, c_r, ca_s, ca_r,
):
    n_ra, n_cb, nz, groups, rows, length, layers, width, chunks = dims
    ny = n_ra // nz
    total_chunks = layers * groups * chunks
    cb_rows = rows // n_cb
    me_ra = lax.axis_index("ra")
    me_cb = lax.axis_index("cb")
    me_z, me_y = me_ra // ny, me_ra % ny

    def weight_copies(layer):
        return [
            pltpu.make_async_copy(src.at[layer], dst.at[layer], w_sem.at[layer, k])
            for k, (src, dst) in enumerate(
                [(gw_hbm, gw_ref), (uw_hbm, uw_ref), (dw_hbm, dw_ref)]
            )
        ]

    for layer in range(layers):
        for copy in weight_copies(layer):
            copy.start()

    barrier = pltpu.get_barrier_semaphore()
    for step in range(1, n_ra):
        pl.semaphore_signal(
            barrier, inc=1, device_id={"ra": lax.rem(me_ra + step, n_ra)}, device_id_type=MESH
        )
    for step in range(1, n_cb):
        pl.semaphore_signal(
            barrier, inc=1, device_id={"cb": lax.rem(me_cb + step, n_cb)}, device_id_type=MESH
        )

    def remote(src, dst, send, recv, **where):
        return pltpu.make_async_remote_copy(
            src_ref=src, dst_ref=dst, send_sem=send, recv_sem=recv,
            device_id=where, device_id_type=MESH,
        )

    def square_copy(g, step):
        return remote(
            sq_own.at[g], sq_in.at[g, step - 1], sq_s.at[g, step - 1], sq_r.at[g, step - 1],
            ra=lax.rem(me_ra + step, n_ra),
        )

    def y_copy(g, i, step):
        to = lax.rem(me_y + step, ny)
        return remote(
            part.at[g, i, to], y_in.at[g, i, step - 1],
            y_s.at[g, i, step - 1], y_r.at[g, i, step - 1], ra=me_z * ny + to,
        )

    side, half_z = me_z % 2, me_z // 2
    my_block = 2 * side + half_z
    near = (me_z + 1 - 2 * side) * ny + me_y
    far = (me_z + 2 - 4 * half_z) * ny + me_y

    def near_copy(g, i):
        return remote(
            zpart.at[g, i, pl.ds(2 * (1 - side), 2)], z_in.at[g, i],
            z_s.at[g, i, 0], z_r.at[g, i, 0], ra=near,
        )

    def far_copy(g, i):
        return remote(
            zfold.at[g, i, 1 - half_z], zf_in.at[g, i],
            z_s.at[g, i, 1], z_r.at[g, i, 1], ra=far,
        )

    def hfar_copy(g, i, block):
        block = hid.at[g, i, me_y, block]
        return remote(block, block, hz_s.at[g, i, 0], hz_r.at[g, i, 0], ra=far)

    def hnear_copy(g, i, first):
        block = hid.at[g, i, me_y, pl.ds(2 * first, 2)]
        return remote(block, block, hz_s.at[g, i, 1], hz_r.at[g, i, 1], ra=near)

    def hy_copy(g, i, step, y):
        to = lax.rem(me_y + step, ny)
        block = hid.at[g, i, y]
        return remote(
            block, block, hy_s.at[g, i, step - 1], hy_r.at[g, i, step - 1], ra=me_z * ny + to
        )

    def c_copy(g, step):
        to = lax.rem(me_cb + step, n_cb)
        return remote(
            c_out.at[g, to], c_in.at[g, step - 1], c_s.at[g, step - 1], c_r.at[g, step - 1], cb=to
        )

    def ca_copy(g, step, block):
        to = lax.rem(me_cb + step, n_cb)
        block = c_all.at[g, block]
        return remote(block, block, ca_s.at[g, step - 1], ca_r.at[g, step - 1], cb=to)

    row_in_seq = lax.broadcasted_iota(jnp.int32, (length, width), 0)

    def prepare(layer, g):
        values = carried[g]
        squares = jnp.sum(values * values, axis=1, keepdims=True)
        sq_own[g] = jnp.transpose(jnp.broadcast_to(squares, (rows, 128)))[:8]
        for step in range(1, n_ra):
            square_copy(g, step).start()
        scaled[g] = (values * gain_ref[layer]).astype(BF16)
        acc[g] = jnp.zeros(acc.shape[1:], F32)

    def scale(g):
        total = sq_own[g]
        for step in range(1, n_ra):
            square_copy(g, step).wait()
            total = total + sq_in[g, step - 1]
        total = jnp.transpose(jnp.concatenate([total] * 16, axis=0))
        inv[g] = lax.rsqrt(total / (n_ra * gain_ref.shape[2]) + EPS)

    def project(layer, g, i):
        cols = pl.ds(pl.multiple_of(i * width, width), width)
        for half, (w_ref, taps) in enumerate([(gw_ref, gt_ref), (uw_ref, ut_ref)]):
            lanes = slice(half * width, (half + 1) * width)
            tmp[...] = jnp.dot(scaled[g], w_ref[layer, :, cols], preferred_element_type=F32)
            tap = [taps[layer, pl.ds(k, 1), cols] for k in range(3)]
            for s in range(rows // length):
                span = slice(s * length, (s + 1) * length)
                pre = tmp[span, :] * inv[g, span, :1]
                last = jnp.where(row_in_seq >= 1, pltpu.roll(pre, 1, 0), 0.0)
                older = jnp.where(row_in_seq >= 2, pltpu.roll(pre, 2, 0), 0.0)
                tmp[span, :] = tap[0] * older + tap[1] * last + tap[2] * pre
            part[g, i, :, :, :, lanes] = tmp[...].astype(BF16).reshape(
                ny, nz, rows // n_ra, width
            )
        for step in range(1, ny):
            y_copy(g, i, step).start()

    def add_y(layer, g, i):
        for step in range(1, ny):
            y_copy(g, i, step).wait_recv()
        value = part[g, i, me_y].astype(F32)
        for step in range(1, ny):
            value = value + y_in[g, i, step - 1].astype(F32)
        zpart[g, i] = value.astype(BF16)
        near_copy(g, i).start()

    def fold(layer, g, i):
        near_copy(g, i).wait_recv()
        value = zpart[g, i, pl.ds(2 * side, 2)].astype(F32) + z_in[g, i].astype(F32)
        zfold[g, i] = value.astype(BF16)
        far_copy(g, i).start()

    def activate(layer, g, i):
        cols = pl.ds(pl.multiple_of(i * width, width), width)
        far_copy(g, i).wait_recv()
        value = zfold[g, i, half_z].astype(F32) + zf_in[g, i].astype(F32)
        gate = value[:, :width] + gb_ref[layer, :, cols]
        up = value[:, width:] + ub_ref[layer, :, cols]
        hid[g, i, me_y, my_block] = (gate / (1.0 + jnp.exp(-gate)) * up).astype(BF16)
        hfar_copy(g, i, my_block).start()

    def spread_z(layer, g, i):
        hfar_copy(g, i, 2 * side + 1 - half_z).wait_recv()
        hnear_copy(g, i, side).start()

    def spread_y(layer, g, i):
        hnear_copy(g, i, 1 - side).wait_recv()
        for step in range(1, ny):
            hy_copy(g, i, step, me_y).start()

    def down(layer, g, i):
        depth = pl.ds(pl.multiple_of(i * width, width), width)
        for step in range(1, ny):
            hy_copy(g, i, step, lax.rem(me_y - step + ny, ny)).wait_recv()
        acc[g] += jnp.dot(
            hid[g, i].reshape(rows, width), dw_ref[layer, depth, :], preferred_element_type=F32
        )

    def reduce_start(layer, g):
        c_out[g] = acc[g].astype(BF16).reshape(c_out.shape[1:])
        for step in range(1, n_cb):
            c_copy(g, step).start()

    def reduce_end(layer, g):
        value = acc[g, pl.ds(pl.multiple_of(me_cb * cb_rows, cb_rows), cb_rows), :]
        for step in range(1, n_cb):
            c_copy(g, step).wait()
            value = value + c_in[g, step - 1].astype(F32)
        c_all[g, me_cb] = value.astype(BF16)
        for step in range(1, n_cb):
            ca_copy(g, step, me_cb).start()

    def finish(layer, g):
        for step in range(1, n_cb):
            ca_copy(g, step, lax.rem(me_cb - step + n_cb, n_cb)).wait_recv()
            ca_copy(g, step, me_cb).wait_send()
        branch = c_all[g].reshape(rows, c_all.shape[3]).astype(F32)
        carried[g] = RESID * carried[g] + branch

        @pl.when(layer < layers - 1)
        def _():
            prepare(layer + 1, g)

    def settle(layer, g):
        def one(i, _):
            for step in range(1, ny):
                y_copy(g, i, step).wait_send()
                hy_copy(g, i, step, me_y).wait_send()
            near_copy(g, i).wait_send()
            far_copy(g, i).wait_send()
            hfar_copy(g, i, my_block).wait_send()
            hnear_copy(g, i, side).wait_send()
            return 0

        lax.fori_loop(0, chunks, one, 0)

        @pl.when(layer < layers - 1)
        def _():
            scale(g)

    carried[...] = tok_ref[...].astype(F32)
    pl.semaphore_wait(barrier, n_ra + n_cb - 2)
    for g in range(groups):
        prepare(0, g)
    for layer in range(layers):
        for copy in weight_copies(layer):
            copy.wait()
    for g in range(groups):
        scale(g)

    def body(t, _):
        for lag, stage in STAGES:
            at = t - lag
            run = at // chunks

            @pl.when((at >= 0) & (at < total_chunks))
            def _():
                stage_of[stage](run // groups, run % groups, at % chunks)

        for lag, stage in TAILS:
            at = t - STAGES[-1][0] - lag
            run = at // chunks

            @pl.when((at >= 0) & (at < total_chunks) & (at % chunks == chunks - 1))
            def _():
                stage_of[stage](run // groups, run % groups)

        return 0

    stage_of = {
        "project": project, "add_y": add_y, "activate": activate, "spread_z": spread_z,
        "spread_y": spread_y, "fold": fold,
        "down": down, "reduce_start": reduce_start, "reduce_end": reduce_end,
        "finish": finish, "settle": settle,
    }
    lax.fori_loop(0, total_chunks + STAGES[-1][0] + TAILS[-1][0], body, 0)
    out_ref[...] = carried[...].astype(out_ref.dtype)


def per_device(n_ra, n_cb, tokens, gain, gw, uw, gt, ut, gb, ub, dw):
    seqs, length, d = tokens.shape
    layers, _, ff = gw.shape
    nz = seqs
    ny = n_ra // nz
    groups = GROUPS
    rows = seqs * length // groups
    pr = rows // n_ra
    width = 256 if ff % 256 == 0 and ff // 256 >= 8 else 128
    chunks = ff // width
    dims = (n_ra, n_cb, nz, groups, rows, length, layers, width, chunks)
    vmem = pl.BlockSpec(memory_space=pltpu.VMEM)
    hbm = pl.BlockSpec(memory_space=pl.ANY)
    dma = pltpu.SemaphoreType.DMA
    ys, zs = max(ny - 1, 1), 2
    scratch = [
        pltpu.VMEM((layers, d, ff), BF16),
        pltpu.VMEM((layers, d, ff), BF16),
        pltpu.VMEM((layers, ff, d), BF16),
        pltpu.VMEM((groups, rows, d), F32),
        pltpu.VMEM((groups, rows, d), BF16),
        pltpu.VMEM((groups, rows, 128), F32),
        pltpu.VMEM((rows, width), F32),
        pltpu.VMEM((groups, rows, d), F32),
        pltpu.VMEM((groups, 8, rows), F32),
        pltpu.VMEM((groups, n_ra - 1, 8, rows), F32),
        pltpu.VMEM((groups, chunks, ny, nz, pr, 2 * width), BF16),
        pltpu.VMEM((groups, chunks, ys, nz, pr, 2 * width), BF16),
        pltpu.VMEM((groups, chunks, nz, pr, 2 * width), BF16),
        pltpu.VMEM((groups, chunks, 2, pr, 2 * width), BF16),
        pltpu.VMEM((groups, chunks, 2, pr, 2 * width), BF16),
        pltpu.VMEM((groups, chunks, pr, 2 * width), BF16),
        pltpu.VMEM((groups, chunks, ny, nz, pr, width), BF16),
        pltpu.VMEM((groups, n_cb, rows // n_cb, d), BF16),
        pltpu.VMEM((groups, n_cb - 1, rows // n_cb, d), BF16),
        pltpu.VMEM((groups, n_cb, rows // n_cb, d), BF16),
        dma((layers, 3)),
        dma((groups, n_ra - 1)), dma((groups, n_ra - 1)),
        dma((groups, chunks, ys)), dma((groups, chunks, ys)),
        dma((groups, chunks, zs)), dma((groups, chunks, zs)),
        dma((groups, chunks, zs)), dma((groups, chunks, zs)),
        dma((groups, chunks, ys)), dma((groups, chunks, ys)),
        dma((groups, n_cb - 1)), dma((groups, n_cb - 1)),
        dma((groups, n_cb - 1)), dma((groups, n_cb - 1)),
    ]
    out = pl.pallas_call(
        functools.partial(kernel, dims),
        out_shape=jax.ShapeDtypeStruct((groups, rows, d), tokens.dtype),
        in_specs=[vmem, vmem, hbm, hbm, vmem, vmem, vmem, vmem, hbm],
        out_specs=vmem,
        scratch_shapes=scratch,
        compiler_params=pltpu.CompilerParams(
            collective_id=0, has_side_effects=True, vmem_limit_bytes=60 * 1024 * 1024
        ),
        name="blocks",
    )(
        tokens.reshape(groups, rows, d), gain[:, None, :], gw, uw, gt, ut,
        gb[:, None, :], ub[:, None, :], dw,
    )
    return out.reshape(tokens.shape)


def solution(mesh):
    in_specs = (
        P(None, None, "ra"),
        P(None, "ra"),
        P(None, "ra", "cb"),
        P(None, "ra", "cb"),
        P(None, None, "cb"),
        P(None, None, "cb"),
        P(None, "cb"),
        P(None, "cb"),
        P(None, "cb", "ra"),
    )
    return jax.shard_map(
        functools.partial(per_device, mesh.shape["ra"], mesh.shape["cb"]),
        mesh=mesh, in_specs=in_specs, out_specs=P(None, None, "ra"), check_vma=False,
    )
```
